32 devices in a mesh: sp: 8 (over z, y), tp: 4 (over x, core).
Axes of the slice: x: 2, y: 2, z: 4, core: 2. Of those that a mesh axis runs over, the one named last changes fastest.
Arguments:
- out_grad: bfloat16 [1024, 2048], P('sp'), may hold values from -6 to 6
- residual: bfloat16 [1024, 2048], P('sp'), may hold values from -6 to 6
- routes: int32 [1024, 2], P('sp'), may hold values from 0 to 3, all different within a row; in each aligned block of 128 rows (0 to 127, 128 to 255, ...) at most 80 rows name the same one
- route_weights: float32 [1024, 2], P('sp'), may hold values from 0.15 to 0.85, as said below
- w_gate: bfloat16 [8, 2048, 2048], P('sp', None, 'tp'), may hold values from -0.125 to 0.125
- w_up: bfloat16 [8, 2048, 2048], P('sp', None, 'tp'), may hold values from -0.125 to 0.125
- w_down: bfloat16 [8, 2048, 2048], P('sp', 'tp'), may hold values from -0.09375 to 0.09375
- out_gate: bfloat16 [1024, 1024], P('sp', 'tp'), may hold values from -6 to 6
- in_gate: bfloat16 [1024, 1024], P('sp', 'tp'), may hold values from -6 to 6
- conv_input: bfloat16 [1024, 1024], P('sp', 'tp'), may hold values from -6 to 6
- conv_out: bfloat16 [1024, 1024], P('sp', 'tp'), may hold values from -6 to 6
- conv_taps: float32 [3, 1024], P(None, 'tp'), may hold values from -3.5 to 3.5
- w_out: bfloat16 [1024, 2048], P('tp'), may hold values from -0.1875 to 0.1875
Outputs:
- grad_resid: bfloat16 [1024, 2048], P('sp')
- grad_up: bfloat16 [8, 2048, 2048], P('sp', None, 'tp')
- grad_down: bfloat16 [8, 2048, 2048], P('sp', 'tp')
- grad_out_gate: bfloat16 [1024, 1024], P('sp', 'tp')
- grad_in_gate: bfloat16 [1024, 1024], P('sp', 'tp')
- grad_conv_input: bfloat16 [1024, 1024], P('sp', 'tp')
- grad_w_out: float32 [2048, 1024], P('sp', 'tp')
The draws below stay inside these ranges and needn't reach their ends.
Inputs may be any that keep to these rules, and one draw needn't show every extreme that they name: `routes`: each row names 2 different experts. In the rows of one index of sp no expert is named more than 80 times, a bound that some block reaches. `route_weights`: the two weights of a row sum to one.
All inputs are finite; a program needn't handle non-finite values.
Results may differ from the reference program's by a relative error of at most 0.013.
Values may be sent and summed in bfloat16 or wider, within the bound.
A program may use at most 128 MiB of HBM per device.

```python
import math
import jax
import jax.numpy as jnp
import numpy as np
from jax import lax

D = 2048
FF_HALF = 2048
SC = 1024
TOP_K = 2
TOK_DEV = 128
TOKENS = 1024
EXPERTS = 4
SLICES = 8
CAP = 80
N_SP = 8
N_TP = 4


def draw_route_weights(key, part):
    leading = jax.random.uniform(key, (TOKENS, 1), jnp.float32, 0.15, 0.85)
    return jnp.concatenate([leading, 1.0 - leading], axis=1)


def with_spikes(array, key, source, target, shards_of, factor):
    owner, partner = [(jnp.arange(array.shape[dim]) // (array.shape[dim] // shards_of)).reshape([-1 if axis == dim else 1 for axis in range(array.ndim)]) for dim in (source, target)]
    chosen = jax.random.permutation(key, shards_of)[partner]
    strong = (owner == chosen) | (owner == (partner + shards_of // 2) % shards_of)
    return jnp.where(strong, factor * array, array)


def steps_of(rng, dims, pieces, least, largest):
    factor_of, own = 1.0, jax.random.fold_in(rng, 6)
    for position, parts in pieces:
        draws = jnp.exp(jax.random.uniform(jax.random.fold_in(own, position), (parts,), jnp.float32, least / len(pieces), largest / len(pieces)))
        factor_of = factor_of * jnp.repeat(draws, dims[position] // parts).reshape([-1 if axis == position else 1 for axis in range(len(dims))])
    return factor_of


def shared_out(own_key, own, number, rows, count, top, reach, lean):
    order = jax.random.permutation(own_key, count)
    heavy_load, usual = load_shares(count, rows * top, reach, lean, True), load_shares(count, rows * top, reach, lean, False)
    places = jnp.arange(count)

    def named(tallies, rotation):
        used = int((tallies > 0).sum())
        fixed = max(1, used // 4)
        passed = fixed + (places - fixed + rotation * (used - fixed)) % max(1, count - fixed)
        return jnp.zeros((count,), jnp.int32).at[order[jnp.where(places < fixed, places, passed)]].set(jnp.asarray(tallies, jnp.int32))

    tallies = jnp.where(number % 4 == 0, named(heavy_load, number // 4), named(usual, number - number // 4 - 1))
    mixed = jax.random.permutation(jax.random.fold_in(own, 3), count)
    source_of, receiver = mixed[0:count // 2 * 2:2], mixed[1:count // 2 * 2:2]
    slack = jnp.minimum(tallies[source_of] - 1, reach - tallies[receiver]) // 2
    slack = jnp.where((source_of == order[0]) | (receiver == order[0]) | (tallies[receiver] == 0), 0, jnp.maximum(slack, 0))
    passed = jax.random.randint(jax.random.fold_in(own, 4), (count // 2,), 0, 1 << 20) % (slack + 1)
    tallies = tallies.at[source_of].add(-passed).at[receiver].add(passed)
    members = jnp.searchsorted(jnp.cumsum(tallies), jnp.arange(rows * top), side="right").astype(jnp.int32)
    grid = members.reshape(top, rows).T
    grid = grid[jax.random.permutation(jax.random.fold_in(own, 1), rows)]
    rotation = jax.random.randint(jax.random.fold_in(own, 2), (rows, 1), 0, top)
    return jnp.take_along_axis(grid, (jnp.arange(top)[None, :] + rotation) % top, axis=1)


def load_shares(amount, total, reach, slope, full):
    portions = [(1 << 20) // math.isqrt(grade ** slope) + 1 for grade in range(1, amount + 1)]
    largest = reach if full else min(reach, max(-(-total // amount), total * portions[0] // sum(portions)))
    least = 1 if total - largest >= amount - 1 else 0
    counts, surplus = [largest] + [least] * (amount - 1), total - largest - least * (amount - 1)
    while surplus > 0:
        candidates = [i for i in range(1, amount) if counts[i] < largest] or [i for i in range(1, amount) if counts[i] < reach]
        whole, remaining = sum([portions[i] for i in candidates]), surplus
        for i in candidates:
            addition = min(reach - counts[i], max(1, remaining * portions[i] // whole), surplus)
            counts[i] = counts[i] + addition
            surplus = surplus - addition
    return np.array(counts)


def scatter_about(key, shape, scale, limit, pieces=(), held_as=jnp.bfloat16):
    entries = scale * jax.random.normal(key, shape, jnp.float32)
    if pieces:
        entries = entries * steps_of(key, shape, pieces, -0.22, 0.18)
    return jnp.clip(entries, -limit, limit).astype(held_as)


def noise_with(stream_key, dims, spread, reach, shards, heavy, kind=jnp.bfloat16):
    entries = spread * jax.random.normal(stream_key, dims, jnp.float32)
    if shards:
        entries = entries * steps_of(stream_key, dims, shards, -0.22, 0.18)
    return jnp.clip(with_spikes(entries, jax.random.fold_in(stream_key, 3), *heavy), -reach, reach).astype(kind)


def setup_inputs(seed: int = 0) -> dict:
    keys = jax.random.split(jax.random.key(seed), 14)
    out_grad = noise_with(keys[0], (TOKENS, D), 1.0, 6.0, ((0, 8),), (0, 1, 8, 2.0))
    residual = scatter_about(keys[1], (TOKENS, D), 1.0, 6.0, ((0, 8),))
    routes_keys = jax.random.split(jax.random.fold_in(keys[2], 1), TOKENS // TOK_DEV)
    routes_turns = jax.random.permutation(jax.random.fold_in(keys[2], 3), TOKENS // TOK_DEV)
    routes = jax.vmap(lambda own, number: shared_out(jax.random.fold_in(keys[2], 2), own, number, TOK_DEV, EXPERTS, TOP_K, CAP, 1))(routes_keys, routes_turns).reshape((TOKENS, TOP_K))
    route_weights = draw_route_weights(jax.random.fold_in(keys[13], 71), 0)
    w_gate = scatter_about(keys[4], (SLICES, D, FF_HALF), D ** -0.5, 0.125, ((0, 8), (2, 4)))
    w_up = scatter_about(keys[5], (SLICES, D, FF_HALF), D ** -0.5, 0.125, ((0, 8), (2, 4)))
    w_down = scatter_about(keys[6], (SLICES, FF_HALF, D), (2 * FF_HALF) ** -0.5, 0.09375, ((0, 8), (1, 4)))
    out_gate = scatter_about(keys[7], (TOKENS, SC), 1.0, 6.0, ((0, 8), (1, 4)))
    in_gate = scatter_about(keys[8], (TOKENS, SC), 1.0, 6.0, ((0, 8), (1, 4)))
    conv_input = scatter_about(keys[9], (TOKENS, SC), 1.0, 6.0, ((0, 8), (1, 4)))
    conv_out = scatter_about(keys[10], (TOKENS, SC), 1.0, 6.0, ((0, 8), (1, 4)))
    conv_taps = scatter_about(keys[11], (3, SC), 3 ** -0.5, 3.5, ((1, 4),), jnp.float32)
    w_out = scatter_about(keys[12], (SC, D), SC ** -0.5, 0.1875, ((0, 4),))
    return dict(out_grad=out_grad, residual=residual, routes=routes, route_weights=route_weights, w_gate=w_gate, w_up=w_up, w_down=w_down, out_gate=out_gate, in_gate=in_gate, conv_input=conv_input, conv_out=conv_out, conv_taps=conv_taps, w_out=w_out)


epsilon = 1e-06

def reference(out_grad, residual, routes, route_weights, w_gate, w_up, w_down, out_gate, in_gate, conv_input, conv_out, conv_taps, w_out):
    resid_f32 = residual.astype(jnp.float32)
    inv_rms = lax.rsqrt(lax.optimization_barrier(jnp.mean(resid_f32 * resid_f32, axis=-1, keepdims=True)) + epsilon)
    unit_rows = resid_f32 * inv_rms
    normed = unit_rows.astype(jnp.bfloat16)
    n_assign = TOKENS * TOP_K
    weighted = (route_weights[:, :, None] * out_grad.astype(jnp.float32)[:, None, :]).astype(jnp.bfloat16).reshape(n_assign, D)
    flat_routes = routes.reshape(-1).astype(jnp.int32)
    onehot = (flat_routes[:, None] == jnp.arange(EXPERTS, dtype=jnp.int32)[None, :]).astype(jnp.int32)
    blocks = onehot.reshape(N_SP, TOP_K * TOK_DEV, EXPERTS)
    before = (jnp.cumsum(blocks, axis=1) - blocks).reshape(n_assign, EXPERTS)
    slot_rank = lax.optimization_barrier(jnp.sum(before * onehot, axis=1)).astype(jnp.int32)
    source = (jnp.arange(n_assign, dtype=jnp.int32) // (TOP_K * TOK_DEV)).astype(jnp.int32)
    slot_table = jnp.full((EXPERTS, N_SP * CAP), n_assign, jnp.int32)
    slot_table = slot_table.at[flat_routes, source * CAP + slot_rank].set(jnp.arange(n_assign, dtype=jnp.int32))
    quarter = FF_HALF // N_TP
    n_blocks = 2 * N_TP

    def one_expert(expert):
        slot_ids = slot_table[expert]
        filled = slot_ids < n_assign
        safe_ids = jnp.where(filled, slot_ids, 0)
        expert_rows = jnp.where(filled[:, None], normed[safe_ids // TOP_K], jnp.zeros((), jnp.bfloat16))
        expert_grads = jnp.where(filled[:, None], weighted[safe_ids], jnp.zeros((), jnp.bfloat16))
        gate_full = jnp.concatenate([w_gate[2 * expert], w_gate[2 * expert + 1]], axis=1)
        up_full = jnp.concatenate([w_up[2 * expert], w_up[2 * expert + 1]], axis=1)
        down_full = jnp.concatenate([w_down[2 * expert], w_down[2 * expert + 1]], axis=0)
        pre_gate = jnp.dot(expert_rows, gate_full, preferred_element_type=jnp.float32)
        pre_up = jnp.dot(expert_rows, up_full, preferred_element_type=jnp.float32)
        sigmoid_gate = jax.nn.sigmoid(pre_gate)
        activated = pre_gate * sigmoid_gate
        hidden = (activated * pre_up).astype(jnp.bfloat16)
        d_hidden = jnp.dot(expert_grads, down_full.T, preferred_element_type=jnp.float32)
        grad_down = jnp.dot(hidden.T, expert_grads, preferred_element_type=jnp.float32).astype(jnp.bfloat16)
        d_gate = (d_hidden * pre_up * sigmoid_gate * (1.0 + pre_gate * (1.0 - sigmoid_gate))).astype(jnp.bfloat16)
        d_up = (d_hidden * activated).astype(jnp.bfloat16)
        grad_up = jnp.dot(expert_rows.T, d_up, preferred_element_type=jnp.float32).astype(jnp.bfloat16)
        partial_value = jnp.einsum('rjf,djf->jrd', d_gate.astype(jnp.float32).reshape(-1, n_blocks, quarter), gate_full.astype(jnp.float32).reshape(D, n_blocks, quarter))
        partial_value = partial_value + jnp.einsum('rjf,djf->jrd', d_up.astype(jnp.float32).reshape(-1, n_blocks, quarter), up_full.astype(jnp.float32).reshape(D, n_blocks, quarter))
        partial_value = lax.optimization_barrier(partial_value.astype(jnp.bfloat16)).astype(jnp.float32)
        slice_sum = lax.optimization_barrier(jnp.sum(partial_value.reshape(2, N_TP, -1, D), axis=1)).astype(jnp.bfloat16)
        down_pair = grad_down.reshape(2, FF_HALF, D)
        up_pair = jnp.transpose(grad_up.reshape(D, 2, FF_HALF), (1, 0, 2))
        return (down_pair, up_pair, slice_sum, slot_ids)
    down_all, up_all, sums_all, ids_all = lax.map(one_expert, jnp.arange(EXPERTS, dtype=jnp.int32))
    grad_down = down_all.reshape(SLICES, FF_HALF, D)
    grad_up = up_all.reshape(SLICES, D, FF_HALF)
    contrib = lax.optimization_barrier(jnp.sum(sums_all.astype(jnp.float32), axis=1)).reshape(-1, D)
    collected = jnp.zeros((n_assign + 1, D), jnp.float32).at[ids_all.reshape(-1)].add(contrib)
    d_normed = lax.optimization_barrier(jnp.sum(collected[:n_assign].reshape(TOKENS, TOP_K, D), axis=1))
    row_mean = lax.optimization_barrier(jnp.mean(unit_rows * d_normed, axis=-1, keepdims=True))
    grad_resid = (out_grad.astype(jnp.float32) + inv_rms * (d_normed - unit_rows * row_mean)).astype(jnp.bfloat16)
    d_mix = jnp.dot(grad_resid, w_out.T, preferred_element_type=jnp.float32)
    conv_f32 = conv_out.astype(jnp.float32)
    gate_f32 = out_gate.astype(jnp.float32)
    grad_out_gate = (d_mix * conv_f32).astype(jnp.bfloat16)
    d_conv = d_mix * gate_f32
    padded = jnp.pad(d_conv, ((1, 1), (0, 0)))
    taps_f32 = conv_taps.astype(jnp.float32)
    d_inner = taps_f32[0] * padded[2:] + taps_f32[1] * padded[1:-1] + taps_f32[2] * padded[:-2]
    grad_in_gate = (d_inner * conv_input.astype(jnp.float32)).astype(jnp.bfloat16)
    grad_conv_input = (d_inner * in_gate.astype(jnp.float32)).astype(jnp.bfloat16)
    mixed = (gate_f32 * conv_f32).astype(jnp.bfloat16)
    grad_w_out = jnp.dot(grad_resid.T, mixed, preferred_element_type=jnp.float32)
    return (grad_resid, grad_up, grad_down, grad_out_gate, grad_in_gate, grad_conv_input, grad_w_out)
```

```python
import functools

import jax
import jax.numpy as jnp
from jax import lax
from jax.experimental import pallas as pl
from jax.experimental.pallas import tpu as pltpu
from jax.sharding import PartitionSpec as P

epsilon = 1e-06


def with_halo(cells, sides, width):
    for axis, dim in sides:
        count = lax.axis_size(axis)
        ends = count - 1
        head = lax.slice_in_dim(cells, 0, width, axis=dim)
        tail = lax.slice_in_dim(cells, cells.shape[dim] - width, cells.shape[dim], axis=dim)
        cells = jnp.concatenate(
            [
                lax.ppermute(tail, axis, [(i, (i + 1) % count) for i in range(ends)]),
                cells,
                lax.ppermute(head, axis, [((i + 1) % count, i) for i in range(ends)]),
            ],
            axis=dim,
        )
    return cells


def per_device_general(
    out_grad,
    residual,
    routes,
    route_weights,
    w_gate,
    w_up,
    w_down,
    out_gate,
    in_gate,
    conv_input,
    conv_out,
    conv_taps,
    w_out,
):
    tok_rows = out_grad.shape[0]
    features = out_grad.shape[1]
    top_count = routes.shape[1]
    slices = lax.axis_size("sp")
    experts = slices // 2
    capacity = 5 * tok_rows // slices
    n_assign = tok_rows * top_count
    resid_f32 = residual.astype(jnp.float32)
    inv_rms = lax.rsqrt(jnp.mean(resid_f32 * resid_f32, axis=-1, keepdims=True) + epsilon)
    unit_rows = resid_f32 * inv_rms
    normed = unit_rows.astype(jnp.bfloat16)
    weighted = (
        (route_weights[:, :, None] * out_grad.astype(jnp.float32)[:, None, :])
        .astype(jnp.bfloat16)
        .reshape(n_assign, features)
    )
    flat_routes = routes.reshape(-1)
    onehot = (flat_routes[:, None] == jnp.arange(experts, dtype=jnp.int32)[None, :]).astype(
        jnp.int32
    )
    slot_rank = jnp.sum((jnp.cumsum(onehot, axis=0) - onehot) * onehot, axis=1)
    slot_index = flat_routes * capacity + slot_rank
    slot_table = (
        jnp.full((experts * capacity,), n_assign, jnp.int32)
        .at[slot_index]
        .set(jnp.arange(n_assign, dtype=jnp.int32))
    )
    filled = slot_table < n_assign
    safe_index = jnp.where(filled, slot_table, 0)
    send_rows = jnp.where(
        filled[:, None], normed[safe_index // top_count], jnp.zeros((), jnp.bfloat16)
    )
    send_grads = jnp.where(filled[:, None], weighted[safe_index], jnp.zeros((), jnp.bfloat16))
    outgoing = jnp.stack([send_rows, send_grads])
    doubled = jnp.repeat(outgoing.reshape(2, experts, capacity, features), 2, axis=1)
    arrived = lax.all_to_all(doubled, "sp", split_axis=1, concat_axis=1, tiled=True)
    expert_rows = arrived[0].reshape(slices * capacity, features)
    expert_grads = arrived[1].reshape(slices * capacity, features)
    gate_local = w_gate[0]
    up_local = w_up[0]
    down_local = w_down[0]
    pre_gate = jnp.dot(expert_rows, gate_local, preferred_element_type=jnp.float32)
    pre_up = jnp.dot(expert_rows, up_local, preferred_element_type=jnp.float32)
    sigmoid_gate = jax.nn.sigmoid(pre_gate)
    activated = pre_gate * sigmoid_gate
    hidden = (activated * pre_up).astype(jnp.bfloat16)
    d_hidden = lax.dot_general(
        expert_grads, down_local, (((1,), (1,)), ((), ())), preferred_element_type=jnp.float32
    )
    grad_down = lax.dot_general(
        hidden, expert_grads, (((0,), (0,)), ((), ())), preferred_element_type=jnp.float32
    ).astype(jnp.bfloat16)
    d_gate = (d_hidden * pre_up * sigmoid_gate * (1.0 + pre_gate * (1.0 - sigmoid_gate))).astype(
        jnp.bfloat16
    )
    d_up = (d_hidden * activated).astype(jnp.bfloat16)
    grad_up = lax.dot_general(
        expert_rows, d_up, (((0,), (0,)), ((), ())), preferred_element_type=jnp.float32
    ).astype(jnp.bfloat16)
    partial_value = lax.dot_general(
        d_gate, gate_local, (((1,), (1,)), ((), ())), preferred_element_type=jnp.float32
    )
    partial_value = partial_value + lax.dot_general(
        d_up, up_local, (((1,), (1,)), ((), ())), preferred_element_type=jnp.float32
    )
    partial_value = partial_value.astype(jnp.bfloat16).reshape(slices, capacity, features)
    summed = lax.psum_scatter(partial_value, "tp", scatter_dimension=2, tiled=True).astype(
        jnp.float32
    )
    returned = lax.all_to_all(
        summed.astype(jnp.bfloat16), "sp", split_axis=0, concat_axis=0, tiled=True
    )
    columns = returned.shape[2]
    flat_back = returned.reshape(slices * capacity, columns)
    first_index = 2 * flat_routes * capacity + slot_rank
    contrib = flat_back[first_index].astype(jnp.float32) + flat_back[first_index + capacity].astype(
        jnp.float32
    )
    d_normed = jnp.sum(contrib.reshape(tok_rows, top_count, columns), axis=1)
    col_start = lax.axis_index("tp") * columns
    unit_part = lax.dynamic_slice_in_dim(unit_rows, col_start, columns, 1)
    grad_part = lax.dynamic_slice_in_dim(out_grad, col_start, columns, 1).astype(jnp.float32)
    row_dots = lax.psum(jnp.sum(unit_part * d_normed, axis=-1), "tp")
    row_mean = row_dots[:, None] / features
    resid_part = (grad_part + inv_rms * (d_normed - unit_part * row_mean)).astype(jnp.bfloat16)
    grad_resid = lax.all_gather(resid_part, "tp", axis=1, tiled=True)
    d_mix = lax.dot_general(
        grad_resid, w_out, (((1,), (1,)), ((), ())), preferred_element_type=jnp.float32
    )
    conv_f32 = conv_out.astype(jnp.float32)
    gate_f32 = out_gate.astype(jnp.float32)
    grad_out_gate = (d_mix * conv_f32).astype(jnp.bfloat16)
    d_conv = d_mix * gate_f32
    padded = with_halo(d_conv.astype(jnp.bfloat16), (("sp", 0),), 1).astype(d_conv.dtype)
    d_inner = conv_taps[0] * padded[2:] + conv_taps[1] * padded[1:-1] + conv_taps[2] * padded[:-2]
    grad_in_gate = (d_inner * conv_input.astype(jnp.float32)).astype(jnp.bfloat16)
    grad_conv_input = (d_inner * in_gate.astype(jnp.float32)).astype(jnp.bfloat16)
    mixed = (gate_f32 * conv_f32).astype(jnp.bfloat16)
    grad_w_out = lax.psum_scatter(
        lax.dot_general(
            grad_resid, mixed, (((0,), (0,)), ((), ())), preferred_element_type=jnp.float32
        ),
        "sp",
        scatter_dimension=0,
        tiled=True,
    )
    return (
        grad_resid,
        grad_up[None],
        grad_down[None],
        grad_out_gate,
        grad_in_gate,
        grad_conv_input,
        grad_w_out,
    )


MESH = pl.DeviceIdType.MESH
BF16 = jnp.bfloat16
F32 = jnp.float32
VMEM_LIMIT = 60 * 1024 * 1024


def place():
    sp, tp = lax.axis_index("sp"), lax.axis_index("tp")
    return sp, tp, lax.div(sp, 2), lax.rem(sp, 2), lax.div(tp, 2), lax.rem(tp, 2)


def greet(peers):
    barrier = pltpu.get_barrier_semaphore()
    for peer in peers:
        pl.semaphore_signal(barrier, inc=1, device_id=peer, device_id_type=MESH)
    return lambda: pl.semaphore_wait(barrier, len(peers))


def columns_of(index, width):
    return pl.ds(pl.multiple_of(index * width, width), width)


def rows_of(index, height):
    return pl.ds(pl.multiple_of(index * height, height), height)


def dispatch_kernel(
    slices, cap, rt, rw, resid, og, ogate, cout,
    rows, grads, mixed, sel,
    send_rows, send_grads, send_sem, recv_sem, local_sem,
):
    sp, tp, z, y, x, c = place()
    pairs = slices // 2
    tok, features = resid.shape
    width = features // 4
    sibling = (sp, 2 * x + 1 - c)
    x_peer = (sp, 2 * (1 - x) + c)
    y_peer = (2 * z + 1 - y, tp)
    sp_peers = [(lax.rem(sp + k, slices), tp) for k in range(1, slices)]
    ready = greet(sp_peers + [sibling, x_peer])

    grid_r = lax.broadcasted_iota(jnp.int32, (tok, tok), 0)
    grid_c = lax.broadcasted_iota(jnp.int32, (tok, tok), 1)
    earlier = (grid_r < grid_c).astype(F32).astype(BF16)
    slot = lax.broadcasted_iota(jnp.int32, (cap, tok), 0).astype(F32)
    r32 = resid[...].astype(F32)
    inv_rms = lax.rsqrt(jnp.mean(r32 * r32, axis=-1, keepdims=True) + epsilon)
    mine = columns_of(tp, width)
    normed = (resid[:, mine].astype(F32) * inv_rms).astype(BF16)
    cot = og[:, mine]
    for e in range(pairs):
        named = (rt[...] == e).astype(F32)
        mask = jnp.sum(named, axis=0, keepdims=True)
        weight = jnp.sum(named * rw[...], axis=0, keepdims=True)
        rank = jnp.dot(
            jnp.broadcast_to(mask, (8, tok)).astype(BF16), earlier, preferred_element_type=F32
        )[0:1]
        pick = jnp.where((rank == slot) & (mask > 0.5), 1.0, 0.0)
        slot_weight = jnp.sum(pick * weight, axis=1, keepdims=True)
        pick = pick.astype(BF16)
        here = slice(e * cap, (e + 1) * cap)
        sel[here, :] = pick
        send_rows[here, :] = jnp.dot(pick, normed, preferred_element_type=F32).astype(BF16)
        send_grads[here, :] = (
            slot_weight * jnp.dot(pick, cot, preferred_element_type=F32)
        ).astype(BF16)
    mixed[rows_of(sp, tok), :] = (ogate[...].astype(F32) * cout[...].astype(F32)).astype(BF16)
    ready()

    started = []

    def send(n, src, dst, peer):
        copy = pltpu.make_async_remote_copy(
            src_ref=src, dst_ref=dst, send_sem=send_sem.at[n], recv_sem=recv_sem.at[n],
            device_id=peer, device_id_type=MESH,
        )
        copy.start()
        started.append(copy)
        return copy

    ours = ((send_rows, rows), (send_grads, grads))

    def block(pair, yy, xx, cc):
        return (rows_of(2 * pair + yy, cap), columns_of(2 * xx + cc, width))

    arriving = {}
    home = block(z, y, x, c)
    for k in range(1, pairs):
        far = lax.rem(z - k + pairs, pairs)
        for a, (src, dst) in enumerate(ours):
            arriving[k, a] = send(
                16 * pairs + 2 * k + a, src.at[rows_of(far, cap), :], dst.at[home],
                (2 * far + y, tp),
            )
    locals_ = []
    for a, (src, dst) in enumerate(ours):
        copy = pltpu.make_async_copy(src.at[rows_of(z, cap), :], dst.at[home], local_sem.at[a])
        copy.start()
        locals_.append(copy)
    for copy in locals_:
        copy.wait()

    def spread(k):
        pair = lax.rem(z + k, pairs)
        at = block(pair, y, x, c)
        out = {}
        for a, (_, dst) in enumerate(ours):
            out["x", a] = send(16 * k + a, dst.at[at], dst.at[at], x_peer)
            out["y", a] = send(16 * k + 2 + a, dst.at[at], dst.at[at], y_peer)
        for a, (_, dst) in enumerate(ours):
            out["s", a] = send(16 * k + 4 + a, dst.at[at], dst.at[at], sibling)
        return out

    def forward(k, out):
        pair = lax.rem(z + k, pairs)
        got_x = block(pair, y, 1 - x, c)
        got_y = block(pair, 1 - y, x, c)
        out["x", 0].wait_recv()
        out["dy"] = send(16 * k + 6, rows.at[got_x], rows.at[got_x], y_peer)
        out["y", 1].wait_recv()
        out["dx"] = send(16 * k + 7, grads.at[got_y], grads.at[got_y], x_peer)
        out["x", 1].wait_recv()
        out["y", 0].wait_recv()
        for a, (_, dst) in enumerate(ours):
            out["sx", a] = send(16 * k + 8 + a, dst.at[got_x], dst.at[got_x], sibling)
            out["sy", a] = send(16 * k + 10 + a, dst.at[got_y], dst.at[got_y], sibling)

    def finish(k, out):
        pair = lax.rem(z + k, pairs)
        got = block(pair, 1 - y, 1 - x, c)
        out["dy"].wait_recv()
        out["sd", 0] = send(16 * k + 12, rows.at[got], rows.at[got], sibling)
        out["dx"].wait_recv()
        out["sd", 1] = send(16 * k + 13, grads.at[got], grads.at[got], sibling)

    outs = []
    for k in range(pairs):
        if k:
            for a in range(2):
                arriving[k, a].wait_recv()
        outs.append(spread(k))
        if k == pairs - 1:
            mixed_copies = [
                send(
                    18 * pairs + j, mixed.at[rows_of(sp, tok), :], mixed.at[rows_of(sp, tok), :],
                    peer,
                )
                for j, peer in enumerate(sp_peers)
            ]
        if k:
            forward(k - 1, outs[k - 1])
        if k > 1:
            finish(k - 2, outs[k - 2])
    forward(pairs - 1, outs[-1])
    finish(pairs - 2, outs[-2])
    finish(pairs - 1, outs[-1])
    for out in outs:
        for kind in ("s", "sx", "sy", "sd"):
            for a in range(2):
                out[kind, a].wait_recv()
    for copy in mixed_copies:
        copy.wait_recv()
    for copy in started:
        copy.wait_send()


def dispatch(slices, cap, rt, rw, resid, og, ogate, cout):
    features, tok = resid.shape[1], resid.shape[0]
    pairs = slices // 2
    vmem = pl.BlockSpec(memory_space=pltpu.VMEM)
    sems = 18 * pairs + slices
    return pl.pallas_call(
        functools.partial(dispatch_kernel, slices, cap),
        out_shape=(
            jax.ShapeDtypeStruct((slices * cap, features), BF16),
            jax.ShapeDtypeStruct((slices * cap, features), BF16),
            jax.ShapeDtypeStruct((slices * tok, ogate.shape[1]), BF16),
            jax.ShapeDtypeStruct((pairs * cap, tok), BF16),
        ),
        in_specs=[vmem] * 6,
        out_specs=[vmem] * 4,
        scratch_shapes=[
            pltpu.VMEM((pairs * cap, features // 4), BF16),
            pltpu.VMEM((pairs * cap, features // 4), BF16),
            pltpu.SemaphoreType.DMA((sems,)),
            pltpu.SemaphoreType.DMA((sems,)),
            pltpu.SemaphoreType.DMA((2,)),
        ],
        compiler_params=pltpu.CompilerParams(
            collective_id=0, has_side_effects=True, vmem_limit_bytes=VMEM_LIMIT
        ),
        name="dispatch",
    )(rt, rw, resid, og, ogate, cout)


def tail_kernel(
    slices, cap, part, sel, resid, og, ogate, igate, cin, cout, taps, wout, mixed,
    gresid, gogate, gigate, gcin, gwout,
    sib, pairsum, plane, zsend, ret, dnq, dn, grx, edge_out, edge_in, send_sem, recv_sem,
):
    sp, tp, z, y, x, c = place()
    pairs = slices // 2
    tok, features = resid.shape
    width = features // 4
    sibling = (sp, 2 * x + 1 - c)
    x_peer = (sp, 2 * (1 - x) + c)
    x_other = (sp, 2 * (1 - x) + 1 - c)
    y_peer = (2 * z + 1 - y, tp)
    diagonal = (2 * z + 1 - y, 2 * (1 - x) + c)
    sp_peers = [(lax.rem(sp + k, slices), tp) for k in range(1, slices)]
    greet(sp_peers + [sibling, x_peer, x_other, diagonal])()
    started = []

    def send(n, src, dst, peer):
        copy = pltpu.make_async_remote_copy(
            src_ref=src, dst_ref=dst, send_sem=send_sem.at[n], recv_sem=recv_sem.at[n],
            device_id=peer, device_id_type=MESH,
        )
        copy.start()
        started.append(copy)
        return copy

    order = list(range(1, pairs)) + [0]
    halves = {}
    for k in order:
        at = rows_of(lax.rem(z + k, pairs), 2 * cap)
        for h in range(2):
            halves[k, h] = send(
                8 * k + h, part.at[at, columns_of(2 * h + 1 - c, width)], sib.at[h, at, :], sibling
            )
    moved = {}
    for k in order:
        pair = lax.rem(z + k, pairs)
        at = rows_of(pair, 2 * cap)
        for h in range(2):
            halves[k, h].wait_recv()
            pairsum[h, at, :] = (
                part[at, columns_of(2 * h + c, width)].astype(F32) + sib[h, at, :].astype(F32)
            ).astype(BF16)
        same, other = rows_of(2 * pair + y, cap), rows_of(2 * pair + 1 - y, cap)
        slots = rows_of(pair, cap)
        moved[k] = [
            send(8 * k + 2, pairsum.at[1 - x, same, :], plane.at[0, slots, :], x_peer),
            send(8 * k + 3, pairsum.at[x, other, :], plane.at[1, slots, :], y_peer),
            send(8 * k + 4, pairsum.at[1 - x, other, :], plane.at[2, slots, :], diagonal),
        ]
    back = []
    for k in order:
        pair = lax.rem(z + k, pairs)
        slots = rows_of(pair, cap)
        for copy in moved[k]:
            copy.wait_recv()
        total = (
            pairsum[x, rows_of(2 * pair + y, cap), :].astype(F32)
            + plane[0, slots, :].astype(F32)
            + plane[1, slots, :].astype(F32)
            + plane[2, slots, :].astype(F32)
        ).astype(BF16)
        if k:
            zsend[slots, :] = total
            back.append(
                send(8 * k + 5, zsend.at[slots, :], ret.at[rows_of(z, cap), :], (2 * pair + y, tp))
            )
        else:
            ret[slots, :] = total
    r32 = resid[...].astype(F32)
    inv_rms = lax.rsqrt(jnp.mean(r32 * r32, axis=-1, keepdims=True) + epsilon)
    for copy in back:
        copy.wait_recv()
    first = 8 * pairs
    quarter = lax.dot_general(
        sel[...], ret[...], (((0,), (0,)), ((), ())), preferred_element_type=F32
    ).astype(BF16)
    dnq[...] = quarter
    mine = columns_of(tp, width)
    dn[:, mine] = quarter
    shares = [
        send(first + n, dnq, dn.at[:, mine], peer)
        for n, peer in enumerate((x_other, x_peer, sibling))
    ]
    for copy in shares:
        copy.wait_recv()
    unit = r32 * inv_rms
    d_normed = dn[...].astype(F32)
    row_mean = jnp.mean(unit * d_normed, axis=-1, keepdims=True)
    gresid[...] = (og[...].astype(F32) + inv_rms * (d_normed - unit * row_mean)).astype(BF16)
    share = features // slices
    first += 3
    across = [
        send(
            first + n, gresid.at[:, columns_of(peer[0], share)], grx.at[rows_of(sp, tok), :], peer
        )
        for n, peer in enumerate(sp_peers)
    ]
    d_mix = lax.dot_general(
        gresid[...], wout[...], (((1,), (1,)), ((), ())), preferred_element_type=F32
    )
    conv = cout[...].astype(F32)
    d_conv = d_mix * ogate[...].astype(F32)
    edge_out[0] = d_conv[tok - 8 :]
    edge_out[1] = d_conv[:8]
    first += slices
    edges = [
        send(first, edge_out.at[0], edge_in.at[0], sp_peers[0]),
        send(first + 1, edge_out.at[1], edge_in.at[1], sp_peers[-1]),
    ]
    grx[rows_of(sp, tok), :] = gresid[:, columns_of(sp, share)]
    gogate[...] = (d_mix * conv).astype(BF16)
    for copy in edges:
        copy.wait_recv()
    before = jnp.where(sp > 0, edge_in[0, 7:8, :], 0.0)
    after = jnp.where(sp < slices - 1, edge_in[1, 0:1, :], 0.0)
    at = lax.broadcasted_iota(jnp.int32, d_conv.shape, 0)
    later = jnp.where(at == tok - 1, after, pltpu.roll(d_conv, tok - 1, 0))
    former = jnp.where(at == 0, before, pltpu.roll(d_conv, 1, 0))
    d_inner = taps[0:1, :] * later + taps[1:2, :] * d_conv + taps[2:3, :] * former
    gigate[...] = (d_inner * cin[...].astype(F32)).astype(BF16)
    gcin[...] = (d_inner * igate[...].astype(F32)).astype(BF16)
    for copy in across:
        copy.wait_recv()
    gwout[...] = lax.dot_general(
        grx[...], mixed[...], (((0,), (0,)), ((), ())), preferred_element_type=F32
    )
    for copy in started:
        copy.wait_send()


def tail(slices, cap, part, sel, resid, og, ogate, igate, cin, cout, taps, wout, mixed):
    tok, features = resid.shape
    channels = ogate.shape[1]
    pairs = slices // 2
    width = features // 4
    vmem = pl.BlockSpec(memory_space=pltpu.VMEM)
    sems = 8 * pairs + 3 + slices + 2
    small = jax.ShapeDtypeStruct((tok, channels), BF16)
    return pl.pallas_call(
        functools.partial(tail_kernel, slices, cap),
        out_shape=(
            jax.ShapeDtypeStruct((tok, features), BF16), small, small, small,
            jax.ShapeDtypeStruct((features // slices, channels), F32),
        ),
        in_specs=[vmem] * 11,
        out_specs=[vmem] * 5,
        scratch_shapes=[
            pltpu.VMEM((2, slices * cap, width), BF16),
            pltpu.VMEM((2, slices * cap, width), BF16),
            pltpu.VMEM((3, pairs * cap, width), BF16),
            pltpu.VMEM((pairs * cap, width), BF16),
            pltpu.VMEM((pairs * cap, width), BF16),
            pltpu.VMEM((tok, width), BF16),
            pltpu.VMEM((tok, features), BF16),
            pltpu.VMEM((slices * tok, features // slices), BF16),
            pltpu.VMEM((2, 8, channels), F32),
            pltpu.VMEM((2, 8, channels), F32),
            pltpu.SemaphoreType.DMA((sems,)),
            pltpu.SemaphoreType.DMA((sems,)),
        ],
        compiler_params=pltpu.CompilerParams(
            collective_id=1, has_side_effects=True, vmem_limit_bytes=VMEM_LIMIT
        ),
        name="tail",
    )(part, sel, resid, og, ogate, igate, cin, cout, taps, wout, mixed)


def per_device(
    out_grad, residual, routes, route_weights, w_gate, w_up, w_down,
    out_gate, in_gate, conv_input, conv_out, conv_taps, w_out,
):
    slices = lax.axis_size("sp")
    cap = 5 * out_grad.shape[0] // slices
    expert_rows, expert_grads, mixed, sel = dispatch(
        slices, cap, routes.T, route_weights.T, residual, out_grad, out_gate, conv_out
    )
    gate_local, up_local, down_local = w_gate[0], w_up[0], w_down[0]
    pre_gate = jnp.dot(expert_rows, gate_local, preferred_element_type=F32)
    pre_up = jnp.dot(expert_rows, up_local, preferred_element_type=F32)
    sigmoid_gate = jax.nn.sigmoid(pre_gate)
    activated = pre_gate * sigmoid_gate
    hidden = (activated * pre_up).astype(BF16)
    d_hidden = lax.dot_general(
        expert_grads, down_local, (((1,), (1,)), ((), ())), preferred_element_type=F32
    )
    grad_down = lax.dot_general(
        hidden, expert_grads, (((0,), (0,)), ((), ())), preferred_element_type=F32
    ).astype(BF16)
    d_gate = (d_hidden * pre_up * sigmoid_gate * (1.0 + pre_gate * (1.0 - sigmoid_gate))).astype(
        BF16
    )
    d_up = (d_hidden * activated).astype(BF16)
    grad_up = lax.dot_general(
        expert_rows, d_up, (((0,), (0,)), ((), ())), preferred_element_type=F32
    ).astype(BF16)
    partial_value = lax.dot_general(
        d_gate, gate_local, (((1,), (1,)), ((), ())), preferred_element_type=F32
    ) + lax.dot_general(d_up, up_local, (((1,), (1,)), ((), ())), preferred_element_type=F32)
    grad_resid, grad_out_gate, grad_in_gate, grad_conv_input, grad_w_out = tail(
        slices, cap, partial_value.astype(BF16), sel, residual, out_grad, out_gate, in_gate,
        conv_input, conv_out, conv_taps, w_out, mixed,
    )
    return (
        grad_resid, grad_up[None], grad_down[None], grad_out_gate, grad_in_gate,
        grad_conv_input, grad_w_out,
    )


def fits_kernels(mesh, tokens):
    slices = mesh.shape["sp"]
    rows = tokens // slices
    return mesh.shape["tp"] == 4 and slices >= 4 and (5 * rows // slices) % 16 == 0


def on_device(mesh, out_grad, *rest):
    tokens = out_grad.shape[0] * mesh.shape["sp"]
    body = per_device if fits_kernels(mesh, tokens) else per_device_general
    return body(out_grad, *rest)


def solution(mesh):
    in_specs = (
        P("sp", None),
        P("sp", None),
        P("sp", None),
        P("sp", None),
        P("sp", None, "tp"),
        P("sp", None, "tp"),
        P("sp", "tp", None),
        P("sp", "tp"),
        P("sp", "tp"),
        P("sp", "tp"),
        P("sp", "tp"),
        P(None, "tp"),
        P("tp", None),
    )
    out_specs = (
        P("sp", None),
        P("sp", None, "tp"),
        P("sp", "tp", None),
        P("sp", "tp"),
        P("sp", "tp"),
        P("sp", "tp"),
        P("sp", "tp"),
    )
    return jax.shard_map(
        functools.partial(on_device, mesh), mesh=mesh, in_specs=in_specs, out_specs=out_specs, check_vma=False
    )
```
